128 devices in a mesh: sp: 16 (over z, x), dp: 8 (over y, core).
Axes of the slice: x: 4, y: 4, z: 4, core: 2. Of those that a mesh axis runs over, the one named last changes fastest.
Arguments:
- queries: bfloat16 [8, 2048, 2048], P('dp', 'sp'), may hold values from -9 to 9
- keys: bfloat16 [8, 2048, 512], P('dp', 'sp'), may hold values from -9 to 9
- values: bfloat16 [8, 2048, 512], P('dp', 'sp'), may hold values from -6 to 6
- out_grad: bfloat16 [8, 2048, 2048], P('dp', 'sp'), may hold values from -24 to 24
- layer_in: bfloat16 [8, 2048, 4096], P('dp', 'sp'), may hold values from -0.09375 to 0.09375
- key_weight: bfloat16 [4096, 512], P('dp'), may hold values from -0.09375 to 0.09375
- value_weight: bfloat16 [4096, 512], P('dp'), may hold values from -0.09375 to 0.09375
- query_gain: float32 [128], replicated, may hold values from 0.64 to 6.04
- key_gain: float32 [128], replicated, may hold values from 0.64 to 6.04
Outputs:
- grad_query: bfloat16 [8, 2048, 2048], P('dp', 'sp')
- grad_in: bfloat16 [8, 2048, 4096], P('dp', 'sp')
- grad_key_weight: float32 [4096, 512], P('dp')
- grad_value_weight: float32 [4096, 512], P('dp')
The draws below stay inside these ranges and needn't reach their ends.
All inputs are finite; a program needn't handle non-finite values.
Results may differ from the reference program's by a relative error of at most 0.018.
The reference program's roundings to bfloat16 on the way count: a program that leaves them out, or rounds other values in their place, can miss the bound.
Values may be sent and summed in bfloat16 or wider, within the bound.
No kernel may reach another device: no remote copies, remote signals or barrier semaphores. Data moves between devices by JAX's collectives and lax.ppermute only.
A program may use at most 128 MiB of HBM per device.

```python
import math
from functools import partial
import jax
import jax.numpy as jnp
from jax import lax

D = 4096
HEADS = 16
KV_HEADS = 4
HEAD_DIM = 128
GRID_W = 64
TOK_DEV = 128
LEN = 2048
SEQS = 8
QW = 2048
KVW = 512
N_SP = 16
N_DP = 8


def gain_values(key, salt):
    base = jax.random.uniform(jax.random.fold_in(key, salt), (HEAD_DIM,), jnp.float32)
    return 0.64 + 0.72 * base


def draw_query_gain(key, part):
    return gain_values(key, 101)


def draw_key_gain(key, part):
    return gain_values(key, 102)


def drawn(key):
    seq_count = N_DP
    length = TOK_DEV * N_SP
    key_base = jnp.clip(jax.random.normal(jax.random.fold_in(key, 11), (seq_count, length, KV_HEADS * HEAD_DIM), jnp.float32), -6.0, 6.0)
    query_base = jnp.clip(jax.random.normal(jax.random.fold_in(key, 12), (seq_count, length, HEADS * HEAD_DIM), jnp.float32), -6.0, 6.0)
    return (jnp.clip(query_base, -9.0, 9.0), jnp.clip(key_base, -9.0, 9.0))


def draw_queries(key, part):
    return drawn(key)[0].astype(jnp.bfloat16)


def draw_keys(key, part):
    return drawn(key)[1].astype(jnp.bfloat16)


def spiked(entries, own_key, source, target, shards_of, factor):
    def block_of(dim):
        return (jnp.arange(entries.shape[dim]) // (entries.shape[dim] // shards_of)).reshape((-1,) + (1,) * (entries.ndim - 1 - dim))

    one_side = jax.random.permutation(own_key, shards_of)[block_of(target)]
    far = (block_of(target) + shards_of // 2) % shards_of
    return jnp.where((block_of(source) == one_side) | (block_of(source) == far), factor * entries, entries)


def level_of(own_key, extent, cuts, least, top_value):
    def one(dim, parts):
        heights = jax.random.uniform(jax.random.fold_in(jax.random.fold_in(own_key, 6), dim), (parts,), jnp.float32, least / len(cuts), top_value / len(cuts))
        return jnp.repeat(jnp.exp(heights), extent[dim] // parts).reshape((-1,) + (1,) * (len(extent) - dim - 1))

    loudness = one(*cuts[0])
    for cut in cuts[1:]:
        loudness = loudness * one(*cut)
    return loudness


def scatter_about(stream_key, dims, scale, reach, cuts=(), kind=jnp.bfloat16):
    values = jax.random.normal(stream_key, dims, jnp.float32) * scale
    if len(cuts) > 0:
        values = level_of(stream_key, dims, cuts, -0.22, 0.18) * values
    return jnp.clip(values, min=-reach, max=reach).astype(kind)


def heavy_noise(own_key, dims, width, most, cuts, heavy, kind=jnp.bfloat16):
    drawn = width * jax.random.normal(own_key, dims, jnp.float32)
    if cuts:
        drawn = drawn * level_of(own_key, dims, cuts, -0.22, 0.18)
    return jnp.clip(spiked(drawn, jax.random.fold_in(own_key, 3), *heavy), -most, most).astype(kind)


def setup_inputs(seed: int = 0) -> dict:
    key_of = jax.random.split(jax.random.key(seed), 10)
    return {
        "queries": draw_queries(jax.random.fold_in(key_of[9], 71), 0),
        "keys": draw_keys(jax.random.fold_in(key_of[9], 71), 0),
        "values": scatter_about(key_of[2], (SEQS, LEN, KVW), 1.0, 6.0, ((0, 8), (1, 16))),
        "out_grad": scatter_about(key_of[3], (SEQS, LEN, QW), 4.0, 24.0, ((0, 8), (1, 16))),
        "layer_in": heavy_noise(key_of[4], (SEQS, LEN, D), (2.0 / (N_DP * N_SP * TOK_DEV) ** 0.5), 0.09375, ((0, 8), (1, 16)), (1, 2, 16, 2.0)),
        "key_weight": scatter_about(key_of[5], (D, KVW), D ** -0.5, 0.09375, ((0, 8),)),
        "value_weight": scatter_about(key_of[6], (D, KVW), D ** -0.5, 0.09375, ((0, 8),)),
        "query_gain": draw_query_gain(jax.random.fold_in(key_of[9], 71), 0),
        "key_gain": draw_key_gain(jax.random.fold_in(key_of[9], 71), 0),
    }


epsilon = 1e-06
rope_base = 10000.0

def norm_rotate(vector, gain_vec, row_index, col_index):
    scaled = vector * lax.rsqrt(lax.optimization_barrier(jnp.mean(vector * vector, axis=-1, keepdims=True)) + epsilon) * gain_vec
    quarter = vector.shape[-1] // 4
    inverse = rope_base ** (-jnp.arange(quarter, dtype=jnp.float32) / quarter)
    pieces = []
    for offset, position in ((0, row_index), (2 * quarter, col_index)):
        angles = position.astype(jnp.float32)[:, None] * inverse[None, :]
        cosine = jnp.cos(angles)
        sine_part = jnp.sin(angles)
        first_half = scaled[:, offset:offset + quarter]
        second_half = scaled[:, offset + quarter:offset + 2 * quarter]
        pieces.append(first_half * cosine - second_half * sine_part)
        pieces.append(first_half * sine_part + second_half * cosine)
    return jnp.concatenate(pieces, axis=1)

def contract_cols(left_side, right_side):
    return lax.dot_general(left_side, right_side, (((1,), (1,)), ((), ())), preferred_element_type=jnp.float32)

def contract_rows(left_side, right_side):
    return lax.dot_general(left_side, right_side, (((0,), (0,)), ((), ())), preferred_element_type=jnp.float32)

def head_grads(query_rows, grad_rows, key_rows, value_rows, query_gain, key_gain):
    length = query_rows.shape[0]
    block_rows = math.gcd(length, 512)
    positions = jnp.arange(length, dtype=jnp.int32)
    row_index = positions // GRID_W
    col_index = positions % GRID_W
    q_rot, q_back = jax.vjp(partial(norm_rotate, gain_vec=query_gain, row_index=row_index, col_index=col_index), query_rows.astype(jnp.float32))
    k_rot, k_back = jax.vjp(partial(norm_rotate, gain_vec=key_gain, row_index=row_index, col_index=col_index), key_rows.astype(jnp.float32))
    q_bf = q_rot.astype(jnp.bfloat16)
    k_bf = k_rot.astype(jnp.bfloat16)
    score_scale = q_rot.shape[-1] ** (-0.5)

    def one_block(accums, block_index):
        k_acc, v_acc = accums
        row_start = block_index * block_rows
        q_block = lax.dynamic_slice_in_dim(q_bf, row_start, block_rows, 0)
        g_block = lax.dynamic_slice_in_dim(grad_rows, row_start, block_rows, 0)
        scores = contract_cols(q_block, k_bf) * score_scale
        shifted = jnp.exp(scores - lax.optimization_barrier(jnp.max(scores, axis=1, keepdims=True)))
        attn_probs = shifted / lax.optimization_barrier(jnp.sum(shifted, axis=1, keepdims=True))
        probs_b = attn_probs.astype(jnp.bfloat16)
        attn_out = jnp.dot(probs_b, value_rows, preferred_element_type=jnp.float32)
        row_delta = lax.optimization_barrier(jnp.sum(g_block.astype(jnp.float32) * attn_out, axis=1, keepdims=True))
        grad_probs = contract_cols(g_block, value_rows)
        grad_scores = (attn_probs * (grad_probs - row_delta)).astype(jnp.bfloat16)
        q_grad = jnp.dot(grad_scores, k_bf, preferred_element_type=jnp.float32) * score_scale
        k_acc = k_acc + contract_rows(grad_scores, q_block) * score_scale
        v_acc = v_acc + contract_rows(probs_b, g_block)
        return ((k_acc, v_acc), q_grad)
    zeros_init = jnp.zeros(query_rows.shape, jnp.float32)
    (k_acc, v_acc), q_grads = lax.scan(one_block, (zeros_init, zeros_init), jnp.arange(length // block_rows, dtype=jnp.int32))
    grad_rq = q_grads.reshape(length, query_rows.shape[1])
    grad_q = q_back(grad_rq)[0].astype(jnp.bfloat16)
    grad_k = k_back(k_acc)[0].astype(jnp.bfloat16)
    return (grad_q, grad_k, v_acc.astype(jnp.bfloat16))

def reference(queries, keys, values, out_grad, layer_in, key_weight, value_weight, query_gain, key_gain):
    seq_count, length, _ = queries.shape
    group_size = HEADS // KV_HEADS

    def by_head(array):
        return array.reshape(seq_count, length, HEADS, HEAD_DIM).transpose(0, 2, 1, 3).reshape(seq_count * HEADS, length, HEAD_DIM)

    def widened(array):
        spread = jnp.broadcast_to(array.reshape(seq_count, length, KV_HEADS, 1, HEAD_DIM), (seq_count, length, KV_HEADS, group_size, HEAD_DIM))
        return by_head(spread.reshape(seq_count, length, HEADS * HEAD_DIM))

    def one_head(items):
        return head_grads(items[0], items[1], items[2], items[3], query_gain, key_gain)
    grad_q, grad_k, grad_v = lax.map(one_head, (by_head(queries), by_head(out_grad), widened(keys), widened(values)))
    grad_query = grad_q.reshape(seq_count, HEADS, length, HEAD_DIM).transpose(0, 2, 1, 3).reshape(seq_count, length, HEADS * HEAD_DIM)

    def grouped(array):
        summed = lax.optimization_barrier(jnp.sum(array.reshape(seq_count, KV_HEADS, group_size, length, HEAD_DIM).astype(jnp.float32), axis=2))
        return summed.astype(jnp.bfloat16).transpose(0, 2, 1, 3).reshape(seq_count * length, KV_HEADS * HEAD_DIM)
    kv_grad = jnp.concatenate([grouped(grad_k), grouped(grad_v)], axis=1)
    both_weights = jnp.concatenate([key_weight, value_weight], axis=1)
    grad_in = contract_cols(kv_grad, both_weights).astype(jnp.bfloat16).reshape(seq_count, length, layer_in.shape[2])
    weight_grad = contract_rows(layer_in.reshape(seq_count * length, layer_in.shape[2]), kv_grad)
    kv_width = KV_HEADS * HEAD_DIM
    return (grad_query, grad_in, weight_grad[:, :kv_width], weight_grad[:, kv_width:])
```

```python
import functools
import math

import jax
import jax.numpy as jnp
import numpy as np
from jax import lax
from jax.experimental import pallas as pl
from jax.experimental.pallas import tpu as pltpu
from jax.sharding import Mesh
from jax.sharding import PartitionSpec as P

HEADS = 16
KV_HEADS = 4
HEAD_DIM = 128
GRID_W = 64
TOK = 128
LEN = 2048
NZ = 4
NX = 4
NY = 4
GROUP_COLS = 512
epsilon = 1e-06
rope_base = 10000.0

F32 = jnp.float32
BF = jnp.bfloat16
SCALE = HEAD_DIM**-0.5
EXP2_SCALE = SCALE * math.log2(math.e)
CHUNK = 512


def rope_tables():
    quarter = HEAD_DIM // 4
    freq = rope_base ** (-np.arange(quarter, dtype=np.float64) / quarter)
    rows = np.arange(LEN // GRID_W)[:, None] * freq[None]
    cols = np.arange(GRID_W)[:, None] * freq[None]
    zr = np.zeros((rows.shape[0], 2 * quarter))
    zc = np.zeros((cols.shape[0], 2 * quarter))
    row_cos = np.concatenate([np.cos(rows), np.cos(rows), zr], 1)
    row_sin = np.concatenate([-np.sin(rows), np.sin(rows), zr], 1)
    col_cos = np.concatenate([zc, np.cos(cols), np.cos(cols)], 1)
    col_sin = np.concatenate([zc, -np.sin(cols), np.sin(cols)], 1)
    return (
        np.stack([row_cos, row_sin]).astype(np.float32),
        np.stack([col_cos, col_sin]).astype(np.float32),
    )


ROW_TABLE, COL_TABLE = rope_tables()
VMEM = pl.BlockSpec(memory_space=pltpu.VMEM)
VMEM_LIMIT = 60 << 20


def call(body, outs, args, name, scratch=(), flops=0, nbytes=1 << 20):
    return pl.pallas_call(
        body,
        out_shape=[jax.ShapeDtypeStruct(s, d) for s, d in outs],
        in_specs=[VMEM] * len(args),
        out_specs=[VMEM] * len(outs),
        scratch_shapes=list(scratch),
        name=name,
        cost_estimate=pl.CostEstimate(flops=flops, bytes_accessed=nbytes, transcendentals=0),
        compiler_params=pltpu.CompilerParams(vmem_limit_bytes=VMEM_LIMIT),
    )(*args)


def axis(name):
    return lax.axis_index(name)


def cyc(i):
    return lax.rem(i, 4)


def span(index, size):
    return pl.ds(pl.multiple_of(index * size, size), size)


def angles(row_ref, col_ref):
    first = 2 * (4 * axis("z") + axis("x"))
    out = []
    for k in range(2):
        halves = [row_ref[k, pl.ds(first + r, 1), :] + col_ref[k] for r in range(2)]
        out.append(jnp.concatenate(halves, axis=0))
    return out


def swap_pairs(v):
    lane = lax.broadcasted_iota(jnp.int32, v.shape, 1)
    return jnp.where(lane % 64 < 32, pltpu.roll(v, 96, 1), pltpu.roll(v, 32, 1))


def rms(u):
    return lax.rsqrt(jnp.mean(u * u, axis=1, keepdims=True) + epsilon)


def forward_rotate(u, gain, cos, sin):
    n = u * rms(u) * gain
    return n * cos + swap_pairs(n) * sin


def backward_rotate(g, u, gain, cos, sin):
    r = rms(u)
    w = (g * cos - swap_pairs(g) * sin) * gain
    return r * w - u * (r * r * r * jnp.mean(u * w, axis=1, keepdims=True))


def prep_body(q_ref, g_ref, k_ref, v_ref, row_ref, col_ref, qg_ref, kg_ref, *outs):
    cos, sin = angles(row_ref, col_ref)
    z = axis("z")
    for s in range(4):
        head = cyc(z + s)
        kv = outs[4 + s]
        u = k_ref[:, span(head, HEAD_DIM)].astype(F32)
        kv[0] = forward_rotate(u, kg_ref[...], cos, sin).astype(BF)
        kv[1] = v_ref[:, span(head, HEAD_DIM)]
    for s in range(4):
        group = cyc(z + s)
        for h in range(4):
            cols = span(4 * group + h, HEAD_DIM)
            rows = pl.ds(h * TOK, TOK)
            u = q_ref[:, cols].astype(F32)
            outs[s][0, rows, :] = forward_rotate(u, qg_ref[...], cos, sin).astype(BF)
            outs[s][1, rows, :] = g_ref[:, cols]


def dg(a, b, ca, cb):
    return lax.dot_general(a, b, (((ca,), (cb,)), ((), ())), preferred_element_type=F32)


def attend_body(*refs):
    q_in, kv_in = refs[0:4], refs[4:8]
    dq_out, dkv_out = refs[8:12], refs[12:16]
    q_all, g_all, k_all, v_all, dq_all, dk_acc, dv_acc = refs[16:]
    for s in range(4):
        rows = pl.ds(s * 512, 512)
        q_all[rows, :] = q_in[s][0]
        g_all[rows, :] = q_in[s][1]
        for t in range(4):
            some = pl.ds(s * 512 + t * TOK, TOK)
            k_all[some, :] = kv_in[s][t, 0]
            v_all[some, :] = kv_in[s][t, 1]
    dk_acc[...] = jnp.zeros_like(dk_acc)
    dv_acc[...] = jnp.zeros_like(dv_acc)

    def step(i, carry):
        rows = span(i, CHUNK)
        q, g, k, v = q_all[rows, :], g_all[rows, :], k_all[...], v_all[...]
        scores = dg(q, k, 1, 1)
        top = jnp.max(scores, axis=1, keepdims=True)
        e = jnp.exp2((scores - top) * EXP2_SCALE)
        probs = e * (1.0 / jnp.sum(e, axis=1, keepdims=True))
        probs_b = probs.astype(BF)
        grad_probs = dg(g, v, 1, 1)
        delta = jnp.sum(probs_b.astype(F32) * grad_probs, axis=1, keepdims=True)
        grad_scores = (probs * (grad_probs - delta)).astype(BF)
        dq_all[rows, :] = (dg(grad_scores, k, 1, 0) * SCALE).astype(BF)
        dk_acc[...] += dg(q, grad_scores, 0, 0)
        dv_acc[...] += dg(g, probs_b, 0, 0)
        return carry

    lax.fori_loop(0, LEN // CHUNK, step, 0)
    for s in range(4):
        rows = pl.ds(s * 512, 512)
        dq_out[s][...] = dq_all[rows, :]
        dkv_out[s][0] = (dk_acc[:, rows].T * SCALE).astype(BF)
        dkv_out[s][1] = dv_acc[:, rows].T.astype(BF)


def sum_four(refs, where):
    total = refs[0][where].astype(F32)
    for r in refs[1:4]:
        total = total + r[where].astype(F32)
    return total


def merge_kv_body(*refs):
    for s in range(4):
        for k in range(2):
            where = (k, pl.ds(s * TOK, TOK), slice(None))
            refs[4 + s][k] = sum_four(refs, where).astype(BF)


def kv_back_body(*refs):
    pieces, (k_ref, row_ref, col_ref, kg_ref, out) = refs[0:4], refs[4:]
    cos, sin = angles(row_ref, col_ref)
    z = axis("z")
    for s in range(4):
        head = cyc(z + s)
        cols = span(head, HEAD_DIM)
        u = k_ref[:, cols].astype(F32)
        g = pieces[s][0].astype(F32)
        out[:, cols] = backward_rotate(g, u, kg_ref[...], cos, sin).astype(BF)
        out[:, span(4 + head, HEAD_DIM)] = pieces[s][1]


def q_back_body(*refs):
    pieces, (q_ref, row_ref, col_ref, qg_ref, out) = refs[0:4], refs[4:]
    cos, sin = angles(row_ref, col_ref)
    z = axis("z")
    for s in range(4):
        group = cyc(z + s)
        for h in range(4):
            cols = span(4 * group + h, HEAD_DIM)
            u = q_ref[:, cols].astype(F32)
            g = pieces[s][pl.ds(h * TOK, TOK), :].astype(F32)
            out[:, cols] = backward_rotate(g, u, qg_ref[...], cos, sin).astype(BF)


def cut_input_body(in_ref, own, sib):
    y, c = axis("y"), axis("c")
    for s in range(4):
        there = cyc(y + s)
        own[s] = in_ref[:, span(2 * there + c, GROUP_COLS)]
        sib[s] = in_ref[:, span(2 * there + 1 - c, GROUP_COLS)]


def weight_body(*refs):
    inputs, own, sib = refs[0:4], refs[4:8], refs[8:12]
    outs = refs[12:16]
    left, right, result = refs[16:]
    for s in range(4):
        for p, kv in ((0, own), (1, sib)):
            rows = pl.ds((2 * s + p) * TOK, TOK)
            left[rows, :] = inputs[s][p]
            right[rows, :] = kv[s][...]
    result[...] = dg(left[...], right[...], 0, 0)
    z = axis("z")
    for s in range(4):
        outs[s][...] = result[span(cyc(z + s), 128), :].astype(BF)


def input_grad_body(*refs):
    own, sib, (kw, vw) = refs[0:4], refs[4:8], refs[8:10]
    own_out, sib_out = refs[10:14], refs[14]
    for s in range(4):
        for kv, out in ((own[s], own_out[s]), (sib[s], sib_out.at[s])):
            both = dg(kv[:, :512], kw[...], 1, 1) + dg(kv[:, 512:], vw[...], 1, 1)
            out[...] = both.astype(BF)


def place_input_body(*refs):
    out = refs[4]
    y, c = axis("y"), axis("c")
    for s in range(4):
        there = cyc(y + s)
        out[:, span(2 * there + c, GROUP_COLS)] = refs[s][0]
        out[:, span(2 * there + 1 - c, GROUP_COLS)] = refs[s][1]


def sum_split_body(*refs):
    x = axis("x")
    for s in range(4):
        where = (span(cyc(x + s), 32), slice(None))
        refs[4 + s][...] = sum_four(refs, where).astype(BF)


def sum_body(*refs):
    refs[4][...] = sum_four(refs, (slice(None), slice(None))).astype(BF)


def place_rows_body(*refs):
    x = axis("x")
    for s in range(4):
        refs[4][span(cyc(x + 4 - s), 32), :] = refs[s][...]


def place_weight_body(*refs):
    z = axis("z")
    for s in range(4):
        rows = span(cyc(z + 4 - s), 128)
        for k in range(2):
            refs[4 + k][rows, :] = refs[s][:, k * 512 : (k + 1) * 512].astype(F32)


def shift(array, name, by):
    n = lax.axis_size(name)
    return lax.ppermute(array, name, [(i, (i + by) % n) for i in range(n)])


def exchange(parts, name, sign=1):
    return [parts[0]] + [shift(parts[s], name, sign * s) for s in (1, 2, 3)]


def on_device(
    queries, keys, values, out_grad, layer_in, key_weight, value_weight, query_gain, key_gain
):
    queries, keys, values, out_grad, layer_in = (
        a[0] for a in (queries, keys, values, out_grad, layer_in)
    )
    qg, kg = query_gain[None], key_gain[None]
    tables = (jnp.asarray(ROW_TABLE), jnp.asarray(COL_TABLE))

    prepared = call(
        prep_body,
        [((2, 512, 128), BF)] * 4 + [((2, 128, 128), BF)] * 4,
        (queries, out_grad, keys, values, *tables, qg, kg),
        "prep",
    )
    kv_pieces = exchange(prepared[4:], "z")
    q_parts = exchange(prepared[:4], "z")
    kv_here = jnp.stack(kv_pieces)
    kv_parts = exchange([kv_here] * 4, "x")

    in_own, in_sib = call(
        cut_input_body, [((4, 128, 512), BF)] * 2, (layer_in,), "cut_input", nbytes=4 << 20
    )
    in_sib = shift(in_sib, "c", 1)
    in_parts = exchange([jnp.stack([in_own[s], in_sib[s]]) for s in range(4)], "y")

    attended = call(
        attend_body,
        [((512, 128), BF)] * 4 + [((2, 512, 128), BF)] * 4,
        (*q_parts, *kv_parts),
        "attend",
        scratch=[pltpu.VMEM((LEN, 128), BF)] * 5 + [pltpu.VMEM((128, LEN), F32)] * 2,
        flops=5 * 2 * LEN * LEN * 128,
        nbytes=4 << 20,
    )
    dkv_parts = exchange(attended[4:], "x", -1)
    dq_parts = exchange(attended[:4], "z", -1)
    merged = call(merge_kv_body, [((2, 128, 128), BF)] * 4, dkv_parts, "merge_kv")
    kv_grads = exchange(merged, "z", -1)
    (kv_sum,) = call(
        kv_back_body, [((128, 1024), BF)], (*kv_grads, keys, *tables, kg), "kv_back"
    )
    (grad_query,) = call(
        q_back_body, [((128, 2048), BF)], (*dq_parts, queries, *tables, qg), "q_back"
    )
    kv_own = exchange([kv_sum] * 4, "y")
    kv_sib = [shift(a, "c", 1) for a in kv_own]

    weight_parts = call(
        weight_body,
        [((128, 1024), BF)] * 4,
        (*in_parts, *kv_own, *kv_sib),
        "weight_grad",
        scratch=[
            pltpu.VMEM((1024, 512), BF),
            pltpu.VMEM((1024, 1024), BF),
            pltpu.VMEM((512, 1024), F32),
        ],
        flops=2 * 1024 * 1024 * 512,
    )
    weight_parts = exchange(weight_parts, "z")
    grads = call(
        input_grad_body,
        [((128, 512), BF)] * 4 + [((4, 128, 512), BF)],
        (*kv_own, *kv_sib, key_weight, value_weight),
        "input_grad",
        flops=2 * 1024 * 1024 * 512,
    )
    grad_sib = shift(grads[4], "c", 1)
    grad_parts = exchange([jnp.stack([grads[s], grad_sib[s]]) for s in range(4)], "y", -1)

    row_parts = call(sum_split_body, [((32, 1024), BF)] * 4, weight_parts, "sum_split")
    row_parts = exchange(row_parts, "x")
    (mine,) = call(sum_body, [((32, 1024), BF)], row_parts, "sum_rows")
    rows = exchange([mine] * 4, "x")
    (rows,) = call(place_rows_body, [((128, 1024), BF)], rows, "place_rows")
    blocks = exchange([rows] * 4, "z")
    (grad_in,) = call(place_input_body, [((128, 4096), BF)], grad_parts, "place_input")
    grad_key_weight, grad_value_weight = call(
        place_weight_body, [((512, 512), F32)] * 2, blocks, "place_weight"
    )
    return (grad_query[None], grad_in[None], grad_key_weight, grad_value_weight)


def solution(mesh):
    cube = Mesh(mesh.devices.reshape(NZ, NX, NY, 2), ("z", "x", "y", "c"))
    sp, dp = ("z", "x"), ("y", "c")
    tokens = P(dp, sp, None)
    weights = P(dp, None)
    return jax.shard_map(
        on_device,
        mesh=cube,
        in_specs=(tokens,) * 5 + (weights,) * 2 + (P(), P()),
        out_specs=(tokens, tokens, weights, weights),
        check_vma=False,
    )
```

```python
import math

import jax
import jax.numpy as jnp
import numpy as np
from jax import lax
from jax.experimental import pallas as pl
from jax.experimental.pallas import tpu as pltpu
from jax.sharding import Mesh
from jax.sharding import PartitionSpec as P


HEAD_DIM = 128
GRID_W = 64
TOK = 128
LEN = 2048
NZ = 4
NX = 4
NY = 4
GROUP_COLS = 512
epsilon = 1e-06
rope_base = 10000.0

F32 = jnp.float32
BF = jnp.bfloat16
SCALE = HEAD_DIM**-0.5
EXP2_SCALE = SCALE * math.log2(math.e)
CHUNK = 512


def rope_tables():
    quarter = HEAD_DIM // 4
    lane = np.arange(HEAD_DIM)
    out = []
    for count, mine in ((LEN // GRID_W, lane < 64), (GRID_W, lane >= 64)):
        shape = (count, HEAD_DIM)
        place = lax.broadcasted_iota(jnp.int32, shape, 1)
        freq = rope_base ** (-(place % quarter).astype(F32) / quarter)
        turn = lax.broadcasted_iota(jnp.int32, shape, 0).astype(F32) * freq
        keep = (place < 64) if mine[0] else (place >= 64)
        sin = jnp.where(place % 64 < quarter, -jnp.sin(turn), jnp.sin(turn))
        out.append(jnp.where(keep, jnp.cos(turn), 0.0))
        out.append(jnp.where(keep, sin, 0.0))
    return out


VMEM = pl.BlockSpec(memory_space=pltpu.VMEM)


def call(body, outs, args, scratch=(), flops=0, nbytes=1 << 20, limit=12):
    return pl.pallas_call(
        body,
        out_shape=[jax.ShapeDtypeStruct(s, d) for s, d in outs],
        in_specs=[VMEM] * len(args),
        out_specs=[VMEM] * len(outs),
        scratch_shapes=list(scratch),
        cost_estimate=pl.CostEstimate(flops=flops, bytes_accessed=nbytes, transcendentals=0),
        compiler_params=pltpu.CompilerParams(vmem_limit_bytes=limit << 20),
    )(*args)


def axis(name):
    return lax.axis_index(name)


def cyc(i):
    return lax.rem(i, 4)


def span(index, size):
    return pl.ds(pl.multiple_of(index * size, size), size)


def angles(tables, z):
    first = 2 * (4 * z + axis("x"))
    out = []
    for row_ref, col_ref in (tables[0::2], tables[1::2]):
        halves = [row_ref[pl.ds(first + r, 1), :] + col_ref[...] for r in range(2)]
        out.append(jnp.concatenate(halves, axis=0))
    return out


def swap_pairs(v):
    lane = lax.broadcasted_iota(jnp.int32, v.shape, 1)
    return jnp.where(lane % 64 < 32, pltpu.roll(v, 96, 1), pltpu.roll(v, 32, 1))


def rms(u):
    return lax.rsqrt(jnp.mean(u * u, axis=1, keepdims=True) + epsilon)


def forward_rotate(u, gain, cos, sin):
    n = u * rms(u) * gain
    return n * cos + swap_pairs(n) * sin


def backward_rotate(g, u, gain, cos, sin):
    r = rms(u)
    w = (g * cos - swap_pairs(g) * sin) * gain
    return r * w - u * (r * r * r * jnp.mean(u * w, axis=1, keepdims=True))


def prep_kv_body(k_ref, v_ref, gain_ref, *refs):
    tables, outs = refs[:4], refs[4:]
    z = axis("z")
    cos, sin = angles(tables, z)
    for s in range(4):
        cols = span(cyc(z + s), HEAD_DIM)
        raw = k_ref[:, cols]
        outs[s][0] = forward_rotate(raw.astype(F32), gain_ref[...], cos, sin).astype(BF)
        outs[s][1] = v_ref[:, cols]
        outs[s][2] = raw


def prep_q_body(q_ref, g_ref, gain_ref, *refs):
    tables, outs = refs[:4], refs[4:]
    z = axis("z")
    cos, sin = angles(tables, z)
    for s in range(4):
        group = cyc(z + s)
        for h in range(4):
            cols = span(4 * group + h, HEAD_DIM)
            rows = pl.ds(h * TOK, TOK)
            u = q_ref[:, cols].astype(F32)
            outs[s][0, rows, :] = forward_rotate(u, gain_ref[...], cos, sin).astype(BF)
            outs[s][1, rows, :] = g_ref[:, cols]


def join_kv_body(*refs):
    kv, raw = refs[4:]
    for s in range(4):
        rows = pl.ds(s * TOK, TOK)
        for k in range(2):
            kv[k, rows, :] = refs[s][k]
        raw[rows, :] = refs[s][2]


def dg(a, b, ca, cb):
    return lax.dot_general(a, b, (((ca,), (cb,)), ((), ())), preferred_element_type=F32)


def attend_body(*refs):
    q_in, kv_in = refs[0:4], refs[4:8]
    dq_out, dk_out, dv_out = refs[8:12], refs[12:16], refs[16:20]
    q_all, g_all, k_all, v_all, dq_all, dk_acc, dv_acc = refs[20:]
    for s in range(4):
        rows = pl.ds(s * 512, 512)
        q_all[rows, :] = q_in[s][0]
        g_all[rows, :] = q_in[s][1]
        k_all[rows, :] = kv_in[s][0]
        v_all[rows, :] = kv_in[s][1]
    dk_acc[...] = jnp.zeros_like(dk_acc)
    dv_acc[...] = jnp.zeros_like(dv_acc)

    def step(i, carry):
        rows = span(i, CHUNK)
        q, g, k, v = q_all[rows, :], g_all[rows, :], k_all[...], v_all[...]
        scores = dg(q, k, 1, 1)
        top = jnp.max(scores, axis=1, keepdims=True)
        e = jnp.exp2((scores - top) * EXP2_SCALE)
        probs = e * (1.0 / jnp.sum(e, axis=1, keepdims=True))
        probs_b = probs.astype(BF)
        grad_probs = dg(g, v, 1, 1)
        delta = jnp.sum(probs_b.astype(F32) * grad_probs, axis=1, keepdims=True)
        grad_scores = (probs * (grad_probs - delta)).astype(BF)
        dq_all[rows, :] = (dg(grad_scores, k, 1, 0) * SCALE).astype(BF)
        dk_acc[...] += dg(q, grad_scores, 0, 0)
        dv_acc[...] += dg(g, probs_b, 0, 0)
        return carry

    lax.fori_loop(0, LEN // CHUNK, step, 0)
    for s in range(4):
        rows = pl.ds(s * 512, 512)
        dq_out[s][...] = dq_all[rows, :]
        dk_out[s][...] = (dk_acc[:, rows].T * SCALE).astype(BF)
        dv_out[s][...] = dv_acc[:, rows].T.astype(BF)


def sum_four(refs, where):
    total = refs[0][where].astype(F32)
    for r in refs[1:4]:
        total = total + r[where].astype(F32)
    return total


def sum_v_body(*refs):
    refs[4][...] = sum_four(refs, (slice(None), slice(None))).astype(BF)


def k_back_body(*refs):
    dq, (v_ref, raw_ref, kg_ref), tables = refs[4:8], refs[8:11], refs[11:15]
    out, msgs = refs[15], refs[16:20]
    z = axis("z")
    for s in range(4):
        rows = pl.ds(s * TOK, TOK)
        cos, sin = angles(tables, cyc(z + 4 - s))
        g = sum_four(refs, (rows, slice(None)))
        u = raw_ref[rows, :].astype(F32)
        k_sum = backward_rotate(g, u, kg_ref[...], cos, sin).astype(BF)
        out[rows, :] = k_sum
        msgs[s][0] = k_sum
        msgs[s][1] = v_ref[rows, :]
        for h in range(4):
            msgs[s][2 + h] = dq[s][pl.ds(h * TOK, TOK), :]


def q_back_body(*refs):
    msgs, (q_ref, qg_ref), tables, out = refs[0:4], refs[4:6], refs[6:10], refs[10]
    z = axis("z")
    cos, sin = angles(tables, z)
    for s in range(4):
        group = cyc(z + s)
        for h in range(4):
            cols = span(4 * group + h, HEAD_DIM)
            u = q_ref[:, cols].astype(F32)
            g = msgs[s][2 + h].astype(F32)
            out[:, cols] = backward_rotate(g, u, qg_ref[...], cos, sin).astype(BF)


def cut_input_body(in_ref, own, sib):
    y, c = axis("y"), axis("c")
    for s in range(4):
        there = cyc(y + s)
        own[s] = in_ref[:, span(2 * there + c, GROUP_COLS)]
        sib[s] = in_ref[:, span(2 * there + 1 - c, GROUP_COLS)]


def weight_body(*refs):
    inputs, own, sib = refs[0:4], refs[4:8], refs[8:12]
    out, right = refs[12:]
    for b in range(4):
        for s in range(4):
            for p, kv in ((0, own), (1, sib)):
                rows = pl.ds(b * 1024 + (2 * s + p) * TOK, TOK)
                right[rows, :] = kv[s][pl.ds(b * TOK, TOK), :]
    total = None
    for b in range(4):
        part = dg(right[pl.ds(b * 1024, 1024), :], inputs[b][...], 0, 0)
        total = part if total is None else total + part
    out[...] = total.astype(BF)


def sum_weight_body(*refs):
    refs[4][...] = sum_four(refs, (slice(None), slice(None))).T.astype(BF)


def place_weight_body(*refs):
    z = axis("z")
    for s in range(4):
        refs[4][:, span(cyc(z + 4 - s), HEAD_DIM)] = refs[s][...].astype(F32)


def input_grad_body(*refs):
    pieces, own, sib = refs[0:4], refs[4:8], refs[8:12]
    out, kv = refs[12:]
    z, y, c = axis("z"), axis("y"), axis("c")
    for s in range(4):
        head = cyc(z + s)
        for k in range(2):
            kv[:, span(4 * k + head, HEAD_DIM)] = pieces[s][k]
    for s in range(4):
        there = cyc(y + 4 - s)
        for w, core in ((own[s], c), (sib[s], 1 - c)):
            both = dg(kv[:, :512], w[0], 1, 1) + dg(kv[:, 512:], w[1], 1, 1)
            out[:, span(2 * there + core, GROUP_COLS)] = both.astype(BF)


def shift(array, name, by):
    n = lax.axis_size(name)
    return lax.ppermute(array, name, [(i, (i + by) % n) for i in range(n)])


def exchange(parts, name, sign=1):
    out = [parts[0]]
    for s in (1, 2, 3):
        out.append(shift(parts[s], name, sign * s))
    return out


def on_device(
    queries, keys, values, out_grad, layer_in, key_weight, value_weight, query_gain, key_gain
):
    return whole(
        *(a[0] for a in (queries, keys, values, out_grad, layer_in)),
        key_weight,
        value_weight,
        query_gain[None],
        key_gain[None],
    )


def whole(queries, keys, values, out_grad, layer_in, key_weight, value_weight, qg, kg):
    square = ((512, 128), BF)
    tables = rope_tables()

    kv_msgs = call(prep_kv_body, [((3, 128, 128), BF)] * 4, (keys, values, kg, *tables))
    kv_pieces = exchange(kv_msgs, "z")
    q_msgs = call(
        prep_q_body, [((2, 512, 128), BF)] * 4, (queries, out_grad, qg, *tables)
    )
    q_parts = exchange(q_msgs, "z")
    kv_here, raw_keys = call(join_kv_body, [((2, 512, 128), BF), square], kv_pieces)
    kv_parts = exchange([kv_here] * 4, "x")

    in_own, in_sib = call(cut_input_body, [((4, 128, 512), BF)] * 2, (layer_in,))
    in_sib = shift(in_sib, "c", 1)
    in_msgs = [None] + [jnp.stack([in_own[s], in_sib[s]]) for s in (1, 2, 3)]
    in_parts = exchange(in_msgs, "y")
    in_first = jnp.stack([in_own[0], in_sib[0]])
    in_all = jnp.stack([in_first, *in_parts[1:]]).reshape(1024, 512)
    inputs = exchange([in_all] * 4, "z")

    weights = jnp.stack([key_weight, value_weight])
    w_prev = shift(weights, "y", 1)
    w_next = shift(weights, "y", -1)
    w_far = jnp.stack([shift(w_prev[0], "y", 1), shift(w_next[1], "y", -1)])
    w_own = [weights, w_prev, w_far, w_next]
    w_sib = [shift(w, "c", 1) for w in w_own]

    attended = call(
        attend_body,
        [square] * 12,
        (*q_parts, *kv_parts),
        scratch=[pltpu.VMEM((LEN, 128), BF)] * 5 + [pltpu.VMEM((128, LEN), F32)] * 2,
        flops=5 * 2 * LEN * LEN * 128,
        nbytes=4 << 20,
        limit=32,
    )
    dq_out, dk_out, dv_out = attended[:4], attended[4:8], attended[8:]
    dv_parts = exchange(dv_out, "x", -1)
    dk_parts = exchange(dk_out, "x", -1)

    (v_sum,) = call(sum_v_body, [square], dv_parts)
    v_own = exchange([v_sum] * 4, "y")
    v_sib = [shift(a, "c", 1) for a in v_own]

    k_sum, *token_grads = call(
        k_back_body,
        [square] + [((6, 128, 128), BF)] * 4,
        (*dk_parts, *dq_out, v_sum, raw_keys, kg, *tables),
    )
    k_own = exchange([k_sum] * 4, "y")
    k_sib = [shift(a, "c", 1) for a in k_own]
    token_grads = exchange(token_grads, "z", -1)

    (grad_query,) = call(
        q_back_body, [((128, 2048), BF)], (*token_grads, queries, qg, *tables)
    )

    def weight_chain(own, sib):
        (part,) = call(
            weight_body,
            [((128, 512), BF)],
            (*inputs, *own, *sib),
            scratch=[pltpu.VMEM((4096, 128), BF)],
            flops=2 * 4096 * 512 * 128,
            limit=16,
        )
        parts = exchange([part] * 4, "x")
        (total,) = call(sum_weight_body, [square], parts)
        blocks = exchange([total] * 4, "z")
        (out,) = call(place_weight_body, [((512, 512), F32)], blocks)
        return out

    grad_value_weight = weight_chain(v_own, v_sib)
    grad_key_weight = weight_chain(k_own, k_sib)
    (grad_in,) = call(
        input_grad_body,
        [((128, 4096), BF)],
        (*token_grads, *w_own, *w_sib),
        scratch=[pltpu.VMEM((128, 1024), BF)],
        flops=2 * 128 * 1024 * 4096,
        nbytes=9 << 20,
        limit=24,
    )
    return (grad_query[None], grad_in[None], grad_key_weight, grad_value_weight)


def solution(mesh):
    cube = Mesh(mesh.devices.reshape(NZ, NX, NY, 2), ("z", "x", "y", "c"))
    sp, dp = ("z", "x"), ("y", "c")
    tokens = P(dp, sp, None)
    weights = P(dp, None)
    return jax.shard_map(
        on_device,
        mesh=cube,
        in_specs=(tokens,) * 5 + (weights,) * 2 + (P(), P()),
        out_specs=(tokens, tokens, weights, weights),
        check_vma=False,
    )
```

```python
import math

import jax
import jax.numpy as jnp
import numpy as np
from jax import lax
from jax.experimental import pallas as pl
from jax.experimental.pallas import tpu as pltpu
from jax.sharding import Mesh
from jax.sharding import PartitionSpec as P


HEAD_DIM = 128
GRID_W = 64
TOK = 128
LEN = 2048
NZ = 4
NX = 4
NY = 4
GROUP_COLS = 512
epsilon = 1e-06
rope_base = 10000.0

F32 = jnp.float32
BF = jnp.bfloat16
SCALE = HEAD_DIM**-0.5
EXP2_SCALE = SCALE * math.log2(math.e)
CHUNK = 1024


def rope_tables():
    quarter = HEAD_DIM // 4
    lane = np.arange(HEAD_DIM)
    out = []
    for count, mine in ((LEN // GRID_W, lane < 64), (GRID_W, lane >= 64)):
        shape = (count, HEAD_DIM)
        place = lax.broadcasted_iota(jnp.int32, shape, 1)
        freq = rope_base ** (-(place % quarter).astype(F32) / quarter)
        turn = lax.broadcasted_iota(jnp.int32, shape, 0).astype(F32) * freq
        keep = (place < 64) if mine[0] else (place >= 64)
        sin = jnp.where(place % 64 < quarter, -jnp.sin(turn), jnp.sin(turn))
        out.append(jnp.where(keep, jnp.cos(turn), 0.0))
        out.append(jnp.where(keep, sin, 0.0))
    return out


VMEM = pl.BlockSpec(memory_space=pltpu.VMEM)


def call(body, outs, args, scratch=(), flops=0, nbytes=1 << 20, limit=12):
    return pl.pallas_call(
        body,
        out_shape=[jax.ShapeDtypeStruct(s, d) for s, d in outs],
        in_specs=[VMEM] * len(args),
        out_specs=[VMEM] * len(outs),
        scratch_shapes=list(scratch),
        cost_estimate=pl.CostEstimate(flops=flops, bytes_accessed=nbytes, transcendentals=0),
        compiler_params=pltpu.CompilerParams(vmem_limit_bytes=limit << 20),
    )(*args)


def axis(name):
    return lax.axis_index(name)


def cyc(i):
    return lax.rem(i, 4)


def span(index, size):
    return pl.ds(pl.multiple_of(index * size, size), size)


def angles(tables, z):
    first = 2 * (4 * z + axis("x"))
    out = []
    for row_ref, col_ref in (tables[0::2], tables[1::2]):
        halves = [row_ref[pl.ds(first + r, 1), :] + col_ref[...] for r in range(2)]
        out.append(jnp.concatenate(halves, axis=0))
    return out


def swap_pairs(v):
    lane = lax.broadcasted_iota(jnp.int32, v.shape, 1)
    return jnp.where(lane % 64 < 32, pltpu.roll(v, 96, 1), pltpu.roll(v, 32, 1))


def rms(u):
    return lax.rsqrt(jnp.mean(u * u, axis=1, keepdims=True) + epsilon)


def forward_rotate(u, gain, cos, sin):
    n = u * rms(u) * gain
    return n * cos + swap_pairs(n) * sin


def backward_rotate(g, u, gain, cos, sin):
    r = rms(u)
    w = (g * cos - swap_pairs(g) * sin) * gain
    return r * w - u * (r * r * r * jnp.mean(u * w, axis=1, keepdims=True))


def prep_kv_body(k_ref, v_ref, gain_ref, *refs):
    tables, outs = refs[:4], refs[4:]
    z = axis("z")
    cos, sin = angles(tables, z)
    for s in range(4):
        cols = span(cyc(z + s), HEAD_DIM)
        raw = k_ref[:, cols]
        outs[s][0] = forward_rotate(raw.astype(F32), gain_ref[...], cos, sin).astype(BF)
        outs[s][1] = v_ref[:, cols]
        outs[s][2] = raw


def prep_q_body(q_ref, g_ref, gain_ref, *refs):
    tables, outs = refs[:4], refs[4:]
    z = axis("z")
    cos, sin = angles(tables, z)
    for s in range(4):
        group = cyc(z + s)
        for h in range(4):
            cols = span(4 * group + h, HEAD_DIM)
            rows = pl.ds(h * TOK, TOK)
            u = q_ref[:, cols].astype(F32)
            outs[s][0, rows, :] = forward_rotate(u, gain_ref[...], cos, sin).astype(BF)
            outs[s][1, rows, :] = g_ref[:, cols]


def join_kv_body(*refs):
    kv, raw = refs[4:]
    for s in range(4):
        rows = pl.ds(s * TOK, TOK)
        for k in range(2):
            kv[k, rows, :] = refs[s][k]
        raw[rows, :] = refs[s][2]


def dg(a, b, ca, cb):
    return lax.dot_general(a, b, (((ca,), (cb,)), ((), ())), preferred_element_type=F32)


def attend_body(*refs):
    q_in, kv_in = refs[0:4], refs[4:8]
    dq_out, dk_out, dv_out = refs[8:12], refs[12:16], refs[16:20]
    q_all, g_all, k_all, v_all, dq_all, dk_acc, dv_acc = refs[20:]
    for s in range(4):
        rows = pl.ds(s * 512, 512)
        q_all[rows, :] = q_in[s][0]
        g_all[rows, :] = q_in[s][1]
        k_all[rows, :] = kv_in[s][0]
        v_all[rows, :] = kv_in[s][1]
    dk_acc[...] = jnp.zeros_like(dk_acc)
    dv_acc[...] = jnp.zeros_like(dv_acc)

    def step(i, carry):
        rows = span(i, CHUNK)
        q, g, k, v = q_all[rows, :], g_all[rows, :], k_all[...], v_all[...]
        scores = dg(q, k, 1, 1)
        top = jnp.max(scores, axis=1, keepdims=True)
        e = jnp.exp2((scores - top) * EXP2_SCALE)
        probs = e * (1.0 / jnp.sum(e, axis=1, keepdims=True))
        probs_b = probs.astype(BF)
        grad_probs = dg(g, v, 1, 1)
        delta = jnp.sum(probs_b.astype(F32) * grad_probs, axis=1, keepdims=True)
        grad_scores = (probs * (grad_probs - delta)).astype(BF)
        dq_all[rows, :] = (dg(grad_scores, k, 1, 0) * SCALE).astype(BF)
        dk_acc[...] += dg(q, grad_scores, 0, 0)
        dv_acc[...] += dg(g, probs_b, 0, 0)
        return carry

    lax.fori_loop(0, LEN // CHUNK, step, 0)
    for s in range(4):
        rows = pl.ds(s * 512, 512)
        dq_out[s][...] = dq_all[rows, :]
        dk_out[s][...] = (dk_acc[:, rows].T * SCALE).astype(BF)
        dv_out[s][...] = dv_acc[:, rows].T.astype(BF)


def sum_four(refs, where):
    total = refs[0][where].astype(F32)
    for r in refs[1:4]:
        total = total + r[where].astype(F32)
    return total


def sum_v_body(*refs):
    refs[4][...] = sum_four(refs, (slice(None), slice(None))).astype(BF)


def k_back_body(*refs):
    dq, (v_ref, raw_ref, kg_ref), tables = refs[4:8], refs[8:11], refs[11:15]
    out, msgs = refs[15], refs[16:20]
    z = axis("z")
    for s in range(4):
        rows = pl.ds(s * TOK, TOK)
        cos, sin = angles(tables, cyc(z + 4 - s))
        g = sum_four(refs, (rows, slice(None)))
        u = raw_ref[rows, :].astype(F32)
        k_sum = backward_rotate(g, u, kg_ref[...], cos, sin).astype(BF)
        out[rows, :] = k_sum
        msgs[s][0] = k_sum
        msgs[s][1] = v_ref[rows, :]
        for h in range(4):
            msgs[s][2 + h] = dq[s][pl.ds(h * TOK, TOK), :]


def q_back_body(*refs):
    msgs, (q_ref, qg_ref), tables, out = refs[0:4], refs[4:6], refs[6:10], refs[10]
    z = axis("z")
    cos, sin = angles(tables, z)
    for s in range(4):
        group = cyc(z + s)
        for h in range(4):
            cols = span(4 * group + h, HEAD_DIM)
            u = q_ref[:, cols].astype(F32)
            g = msgs[s][2 + h].astype(F32)
            out[:, cols] = backward_rotate(g, u, qg_ref[...], cos, sin).astype(BF)


def cut_input_body(in_ref, *outs):
    for s in range(4):
        outs[s][...] = in_ref[:, span(cyc(axis("y") + s), 1024)]


def weight_body(*refs):
    inputs, kv = refs[0:4], refs[4:8]
    own, sib, right = refs[8:]
    for b in range(4):
        for s in range(4):
            rows = pl.ds(b * 512 + s * TOK, TOK)
            right[rows, :] = kv[s][pl.ds(b * TOK, TOK), :]
    core = axis("c")
    for out, which in ((sib, 1 - core), (own, core)):
        total = None
        for b in range(4):
            left = right[pl.ds(b * 512, 512), :]
            part = dg(left, inputs[b][:, span(which, GROUP_COLS)], 0, 0)
            total = part if total is None else total + part
        out[...] = total.astype(out.dtype)


def pair_sum_body(own, sib, out):
    out[...] = (own[...] + sib[...].astype(F32)).astype(BF)


def sum_weight_body(*refs):
    refs[4][...] = sum_four(refs, (slice(None), slice(None))).T.astype(BF)


def place_weight_body(*refs):
    z = axis("z")
    for s in range(4):
        refs[4][:, span(cyc(z + 4 - s), HEAD_DIM)] = refs[s][...].astype(F32)


def input_grad_body(*refs):
    pieces, own, sib = refs[0:4], refs[4:8], refs[8:12]
    out, kv = refs[12:]
    z, y, c = axis("z"), axis("y"), axis("c")
    for s in range(4):
        head = cyc(z + s)
        for k in range(2):
            kv[:, span(4 * k + head, HEAD_DIM)] = pieces[s][k]
    for s in range(4):
        there = cyc(y + 4 - s)
        for w, core in ((own[s], c), (sib[s], 1 - c)):
            both = dg(kv[:, :512], w[0], 1, 1) + dg(kv[:, 512:], w[1], 1, 1)
            out[:, span(2 * there + core, GROUP_COLS)] = both.astype(BF)


def shift(array, name, by):
    n = lax.axis_size(name)
    return lax.ppermute(array, name, [(i, (i + by) % n) for i in range(n)])


def exchange(parts, name, sign=1):
    out = [parts[0]]
    for s in (1, 2, 3):
        out.append(shift(parts[s], name, sign * s))
    return out


def on_device(
    queries, keys, values, out_grad, layer_in, key_weight, value_weight, query_gain, key_gain
):
    return whole(
        *(a[0] for a in (queries, keys, values, out_grad, layer_in)),
        key_weight,
        value_weight,
        query_gain[None],
        key_gain[None],
    )


def whole(queries, keys, values, out_grad, layer_in, key_weight, value_weight, qg, kg):
    square = ((512, 128), BF)
    tables = rope_tables()

    kv_msgs = call(prep_kv_body, [((3, 128, 128), BF)] * 4, (keys, values, kg, *tables))
    kv_pieces = exchange(kv_msgs, "z")
    q_msgs = call(
        prep_q_body, [((2, 512, 128), BF)] * 4, (queries, out_grad, qg, *tables)
    )
    q_parts = exchange(q_msgs, "z")
    kv_here, raw_keys = call(join_kv_body, [((2, 512, 128), BF), square], kv_pieces)
    kv_parts = exchange([kv_here] * 4, "x")

    cuts = call(cut_input_body, [((128, 1024), BF)] * 4, (layer_in,))
    in_parts = exchange(cuts, "y")
    inputs = exchange([jnp.concatenate(in_parts)] * 4, "z")

    weights = jnp.stack([key_weight, value_weight])
    w_prev = shift(weights, "y", 1)
    w_next = shift(weights, "y", -1)
    w_far = jnp.stack([shift(w_prev[0], "y", 1), shift(w_next[1], "y", -1)])
    w_own = [weights, w_prev, w_far, w_next]
    w_sib = [shift(w, "c", 1) for w in w_own]

    attended = call(
        attend_body,
        [square] * 12,
        (*q_parts, *kv_parts),
        scratch=[pltpu.VMEM((LEN, 128), BF)] * 5 + [pltpu.VMEM((128, LEN), F32)] * 2,
        flops=5 * 2 * LEN * LEN * 128,
        nbytes=4 << 20,
        limit=44,
    )
    dq_out, dk_out, dv_out = attended[:4], attended[4:8], attended[8:]
    dv_parts = exchange(dv_out, "x", -1)
    dk_parts = exchange(dk_out, "x", -1)

    (v_sum,) = call(sum_v_body, [square], dv_parts)
    v_own = exchange([v_sum] * 4, "y")

    k_sum, *token_grads = call(
        k_back_body,
        [square] + [((6, 128, 128), BF)] * 4,
        (*dk_parts, *dq_out, v_sum, raw_keys, kg, *tables),
    )
    k_own = exchange([k_sum] * 4, "y")
    token_grads = exchange(token_grads, "z", -1)

    (grad_query,) = call(
        q_back_body, [((128, 2048), BF)], (*token_grads, queries, qg, *tables)
    )

    wide = (128, 512)

    def weight_chain(kv):
        own, sib = call(
            weight_body,
            [(wide, F32), (wide, BF)],
            (*inputs, *kv),
            scratch=[pltpu.VMEM((2048, 128), BF)],
            flops=2 * 4096 * 512 * 128,
            limit=16,
        )
        sib = shift(sib, "c", 1)
        (part,) = call(pair_sum_body, [(wide, BF)], (own, sib))
        parts = exchange([part] * 4, "x")
        (total,) = call(sum_weight_body, [square], parts)
        blocks = exchange([total] * 4, "z")
        (out,) = call(place_weight_body, [((512, 512), F32)], blocks)
        return out

    grad_value_weight = weight_chain(v_own)
    grad_key_weight = weight_chain(k_own)
    (grad_in,) = call(
        input_grad_body,
        [((128, 4096), BF)],
        (*token_grads, *w_own, *w_sib),
        scratch=[pltpu.VMEM((128, 1024), BF)],
        flops=2 * 128 * 1024 * 4096,
        nbytes=9 << 20,
        limit=24,
    )
    return (grad_query[None], grad_in[None], grad_key_weight, grad_value_weight)


def solution(mesh):
    cube = Mesh(mesh.devices.reshape(NZ, NX, NY, 2), ("z", "x", "y", "c"))
    sp, dp = ("z", "x"), ("y", "c")
    tokens = P(dp, sp, None)
    weights = P(dp, None)
    return jax.shard_map(
        on_device,
        mesh=cube,
        in_specs=(tokens,) * 5 + (weights,) * 2 + (P(), P()),
        out_specs=(tokens, tokens, weights, weights),
        check_vma=False,
    )
```
